32 devices in a mesh: ep: 8 (over z, x), tp: 4 (over y, core).
Axes of the slice: x: 2, y: 2, z: 4, core: 2. Of those that a mesh axis runs over, the one named last changes fastest.
Arguments:
- initial_micro_probes: bfloat16 [2048, 2048], P('ep', 'tp'), may hold values from -6 to 6
- initial_micro_lookup_keys: bfloat16 [2048, 2048], P('ep', 'tp'), may hold values from -6 to 6
- initial_micro_payloads: bfloat16 [2048, 2048], P('ep', 'tp'), may hold values from -6 to 6
- result_switch_preactivation: bfloat16 [2048, 2048], P('ep', 'tp'), may hold values from -6 to 6
- insertion_power_preactivation: float32 [2048, 16], P('ep', 'tp'), may hold values from -6 to 6
- fading_preactivation: float32 [2048, 16], P('ep', 'tp'), may hold values from -4.5 to 4.5
- extra_fading_term: float32 [2048, 16], P('ep', 'tp'), may hold values from -0.7 to 0
- channel_fading_speed: float32 [16], P('tp'), may hold values from 2.4414063e-05 to 0.04
- result_scaling_vector: float32 [128], replicated, may hold values from 0.1 to 1.9
- result_mapping_weights: bfloat16 [2048, 2048], P('tp'), may hold values from -0.125 to 0.125
- latter_micro_entries: bfloat16 [1024, 2048], P('ep'), may hold values from -6 to 6
- specialist_scaling_vector: float32 [2048], replicated, may hold values from 0.1 to 1.9
- selected_specialists: int32 [1024, 2], P('ep'), may hold values from 0 to 7, all different within a row; in each aligned block of 128 rows (0 to 127, 128 to 255, ...) at most 64 rows name the same one
- selected_dispatch_weights: float32 [1024, 2], P('ep'), may hold values from 0.1 to 1
- specialist_switch_weights: bfloat16 [8, 2048, 4096], P('ep', None, 'tp'), may hold values from -0.125 to 0.125
- specialist_expand_weights: bfloat16 [8, 2048, 4096], P('ep', None, 'tp'), may hold values from -0.125 to 0.125
- specialist_contract_weights: bfloat16 [8, 4096, 2048], P('ep', 'tp'), may hold values from -0.09375 to 0.09375
Outputs:
- mixer_out: bfloat16 [2048, 2048], P(('ep', 'tp'))
- moe_out: bfloat16 [1024, 2048], P('ep')
The draws below stay inside these ranges and needn't reach their ends.
Inputs may be any that keep to these rules, and one draw needn't show every extreme that they name: `selected_specialists`: each row names 2 different experts. Among the 128 rows of one index of ep no expert is named by more than 64 rows, a bound that some block reaches.
All inputs are finite; a program needn't handle non-finite values.
Results may differ from the reference program's by a relative error of at most 0.024.
Values may be sent and summed in bfloat16 or wider, within the bound.
A program may use at most 64 MiB of HBM per device.

```python
import math
from functools import partial
import jax
import jax.numpy as jnp
import numpy as np
from jax import lax

D = 2048
HEADS = 16
DK = 128
DV = 128
FF = 4096
TOP = 2
BLK = 64
TOK_MIX = 256
TOK_MOE = 128
SEQ_A = 2048
TOKENS_B = 1024
EXPERTS = 8
CAP = 64
N_EP = 8
N_TP = 4


def draw_channel_fading_speed(key, part):
    coin_key, slow_key, fast_key = jax.random.split(jax.random.fold_in(key, 11), 3)
    coins = jax.random.randint(coin_key, (HEADS,), 0, 10)
    fast_heads = coins < 5
    slow = jnp.exp(jax.random.uniform(slow_key, (HEADS,), jnp.float32, jnp.log(0.05), jnp.log(0.5))) / SEQ_A
    fast = jnp.exp(jax.random.uniform(fast_key, (HEADS,), jnp.float32, jnp.log(0.015), jnp.log(0.04)))
    return jnp.where(fast_heads, fast, slow).astype(jnp.float32)


def draw_fading_preactivation(key, part):
    noise_key, shift_key = jax.random.split(jax.random.fold_in(key, 12), 2)
    spans = SEQ_A // TOK_MIX
    noise = jax.random.normal(noise_key, (spans, TOK_MIX, HEADS), jnp.float32)
    shift = jax.random.uniform(shift_key, (spans, 1, HEADS), jnp.float32, -1.5, 1.5)
    return jnp.clip(noise + shift, -4.5, 4.5).reshape(SEQ_A, HEADS).astype(jnp.float32)


def draw_extra_fading_term(key, part):
    place_key, amount_key = jax.random.split(jax.random.fold_in(key, 13), 2)
    places = jax.random.randint(place_key, (3, HEADS), 0, SEQ_A)
    amounts = jnp.log(jax.random.uniform(amount_key, (3, HEADS), jnp.float32, 0.5, 0.8))
    head_ids = jnp.broadcast_to(jnp.arange(HEADS)[None, :], (3, HEADS))
    return jnp.zeros((SEQ_A, HEADS), jnp.float32).at[places, head_ids].min(amounts)


def steps_of(key, dims, cuts, least, high):
    def one(dim, parts):
        draws = jax.random.uniform(jax.random.fold_in(jax.random.fold_in(key, 6), dim), (parts,), jnp.float32, least / len(cuts), high / len(cuts))
        return jnp.repeat(jnp.exp(draws), dims[dim] // parts).reshape((-1,) + (1,) * (len(dims) - dim - 1))

    factor_of = one(*cuts[0])
    for cut in cuts[1:]:
        factor_of = factor_of * one(*cut)
    return factor_of


def deal_out(own_key, own, number, rows, count, top, limit, slope):
    ranking = jax.random.permutation(own_key, count)
    heavy_load, common = portions_of(count, rows * top, limit, slope, True), portions_of(count, rows * top, limit, slope, False)
    places = jnp.arange(count)

    def named(sizes, offset_by):
        used = int((sizes > 0).sum())
        fixed = max(1, used // 4)
        shifted = fixed + (places - fixed + offset_by * (used - fixed)) % max(1, count - fixed)
        return jnp.zeros((count,), jnp.int32).at[ranking[jnp.where(places < fixed, places, shifted)]].set(jnp.asarray(sizes, jnp.int32))

    sizes = jnp.where(number % 4 == 0, named(heavy_load, number // 4), named(common, number - number // 4 - 1))
    mixed = jax.random.permutation(jax.random.fold_in(own, 3), count)
    giver, taker = mixed[0:count // 2 * 2:2], mixed[1:count // 2 * 2:2]
    room = jnp.minimum(sizes[giver] - 1, limit - sizes[taker]) // 2
    room = jnp.where((giver == ranking[0]) | (taker == ranking[0]) | (sizes[taker] == 0), 0, jnp.maximum(room, 0))
    shifted = jax.random.randint(jax.random.fold_in(own, 4), (count // 2,), 0, 1 << 20) % (room + 1)
    sizes = sizes.at[giver].add(-shifted).at[taker].add(shifted)
    items = jnp.searchsorted(jnp.cumsum(sizes), jnp.arange(rows * top), side="right").astype(jnp.int32)
    listing = items.reshape(top, rows).T
    listing = listing[jax.random.permutation(jax.random.fold_in(own, 1), rows)]
    offset_by = jax.random.randint(jax.random.fold_in(own, 2), (rows, 1), 0, top)
    return jnp.take_along_axis(listing, (jnp.arange(top)[None, :] + offset_by) % top, axis=1)


def portions_of(amount, total, most, slope, full):
    loads = [(1 << 20) // math.isqrt(standing ** slope) + 1 for standing in range(1, amount + 1)]
    largest = most if full else min(most, max(-(-total // amount), total * loads[0] // sum(loads)))
    least = 1 if total - largest >= amount - 1 else 0
    given, spare = [largest] + [least] * (amount - 1), total - largest - least * (amount - 1)
    while spare > 0:
        movable = [i for i in range(1, amount) if given[i] < largest] or [i for i in range(1, amount) if given[i] < most]
        pool, remaining = sum([loads[i] for i in movable]), spare
        for i in movable:
            addition = min(most - given[i], max(1, remaining * loads[i] // pool), spare)
            given[i] = given[i] + addition
            spare = spare - addition
    return np.array(given)


def scatter_about(rng, shape, width, limit, cuts=(), kind=jnp.bfloat16):
    array = jax.random.normal(rng, shape, jnp.float32) * width
    if len(cuts) > 0:
        array = steps_of(rng, shape, cuts, -0.22, 0.18) * array
    return jnp.clip(array, min=-limit, max=limit).astype(kind)


def setup_inputs(seed: int = 0) -> dict:
    streams_of = jax.random.split(jax.random.key(seed), 18)
    initial_micro_probes = scatter_about(streams_of[0], (SEQ_A, HEADS * DK), 1.0, 6.0, ((0, 8), (1, 4)))
    initial_micro_lookup_keys = scatter_about(streams_of[1], (SEQ_A, HEADS * DK), 1.0, 6.0, ((0, 8), (1, 4)))
    initial_micro_payloads = scatter_about(streams_of[2], (SEQ_A, HEADS * DV), 1.0, 6.0, ((0, 8), (1, 4)))
    result_switch_preactivation = scatter_about(streams_of[3], (SEQ_A, HEADS * DV), 1.0, 6.0, ((0, 8), (1, 4)))
    insertion_power_preactivation = scatter_about(streams_of[4], (SEQ_A, HEADS), 1.0, 6.0, ((0, 8), (1, 4)), jnp.float32)
    fading_preactivation = draw_fading_preactivation(jax.random.fold_in(streams_of[17], 71), 0)
    extra_fading_term = draw_extra_fading_term(jax.random.fold_in(streams_of[17], 71), 0)
    channel_fading_speed = draw_channel_fading_speed(jax.random.fold_in(streams_of[17], 71), 0)
    result_scaling_vector = jnp.clip(1.0 + 0.18 * jax.random.normal(streams_of[8], (DV,), jnp.float32), 0.1, 1.9)
    result_mapping_weights = scatter_about(streams_of[9], (HEADS * DV, D), (HEADS * DV) ** -0.5, 0.125, ((0, 4),))
    latter_micro_entries = scatter_about(streams_of[10], (TOKENS_B, D), 1.0, 6.0, ((0, 8),))
    specialist_scaling_vector = jnp.clip(1.0 + 0.18 * jax.random.normal(streams_of[11], (D,), jnp.float32), 0.1, 1.9)
    selected_specialists_keys = jax.random.split(jax.random.fold_in(streams_of[12], 1), TOKENS_B // TOK_MOE)
    selected_specialists_turns = jax.random.permutation(jax.random.fold_in(streams_of[12], 3), TOKENS_B // TOK_MOE)
    selected_specialists = jax.vmap(lambda own, number: deal_out(jax.random.fold_in(streams_of[12], 2), own, number, TOK_MOE, EXPERTS, TOP, CAP, 2))(selected_specialists_keys, selected_specialists_turns).reshape((TOKENS_B, TOP))
    selected_dispatch_weights = jnp.clip(0.1 + 0.9 * jax.random.uniform(streams_of[13], (TOKENS_B, TOP), jnp.float32) ** steps_of(streams_of[13], (TOKENS_B, TOP), ((0, 8),), -0.2, 0.2), 0.1, 1.0)
    specialist_switch_weights = scatter_about(streams_of[14], (EXPERTS, D, FF), D ** -0.5, 0.125, ((0, 8), (2, 4)))
    specialist_expand_weights = scatter_about(streams_of[15], (EXPERTS, D, FF), D ** -0.5, 0.125, ((0, 8), (2, 4)))
    specialist_contract_weights = scatter_about(streams_of[16], (EXPERTS, FF, D), FF ** -0.5, 0.09375, ((0, 8), (1, 4)))
    return {"initial_micro_probes": initial_micro_probes, "initial_micro_lookup_keys": initial_micro_lookup_keys, "initial_micro_payloads": initial_micro_payloads, "result_switch_preactivation": result_switch_preactivation, "insertion_power_preactivation": insertion_power_preactivation, "fading_preactivation": fading_preactivation, "extra_fading_term": extra_fading_term, "channel_fading_speed": channel_fading_speed, "result_scaling_vector": result_scaling_vector, "result_mapping_weights": result_mapping_weights, "latter_micro_entries": latter_micro_entries, "specialist_scaling_vector": specialist_scaling_vector, "selected_specialists": selected_specialists, "selected_dispatch_weights": selected_dispatch_weights, "specialist_switch_weights": specialist_switch_weights, "specialist_expand_weights": specialist_expand_weights, "specialist_contract_weights": specialist_contract_weights}


EPS = 1e-06

def exact_product(left, right):
    return jnp.matmul(left, right, precision=lax.Precision.HIGHEST)

def flipped(matrix):
    return jnp.swapaxes(matrix, -1, -2)

def unit_length(values):
    wide = values.astype(jnp.float32)
    return wide * lax.rsqrt(lax.optimization_barrier(jnp.sum(wide * wide, axis=-1, keepdims=True)) + EPS)

def to_blocks(values, block_count):
    shaped = values.reshape(block_count, values.shape[0] // block_count, values.shape[1], values.shape[2])
    return jnp.transpose(shaped, (0, 2, 1, 3))

def unit_inverse(lower):
    size = lower.shape[-1]
    identity = jnp.eye(size, dtype=jnp.float32)
    power = -lower
    result = identity + power
    reach = 2
    while reach < size:
        power = exact_product(power, power)
        result = exact_product(result, identity + power)
        reach = reach * 2
    return result

def block_terms(query, key, value, write, fading_exponent):
    size = query.shape[2]
    running = jnp.cumsum(fading_exponent, axis=-1)
    last = running[..., -1:]
    row_ids = lax.broadcasted_iota(jnp.int32, (size, size), 0)
    col_ids = lax.broadcasted_iota(jnp.int32, (size, size), 1)
    inclusive = row_ids >= col_ids
    strict = row_ids > col_ids
    spread = running[..., :, None] - running[..., None, :]
    fading = jnp.where(inclusive, jnp.exp(jnp.where(inclusive, spread, 0.0)), 0.0)
    key_write = key * write[..., None]
    lower = jnp.where(strict, exact_product(key_write, flipped(key)) * fading, 0.0)
    inverse = unit_inverse(lower)
    update = exact_product(inverse, value * write[..., None])
    erase = exact_product(inverse, key_write * jnp.exp(running)[..., None])
    scores = exact_product(query, flipped(key)) * fading
    query_fade = query * jnp.exp(running)[..., None]
    key_fade = key * jnp.exp(last - running)[..., None]
    return (update, erase, scores, query_fade, key_fade, jnp.exp(last))

def advance(state, inputs):
    update, erase, scores, query_fade, key_fade, block_fade = inputs
    fresh = update - exact_product(erase, state)
    reads = exact_product(query_fade, state) + exact_product(scores, fresh)
    state = state * block_fade[..., None] + exact_product(flipped(key_fade), fresh)
    return (state, reads)

def gated_norm(reads, result_switch_preactivation, result_scaling_vector):
    row_count, head_count, value_width = reads.shape
    scale = lax.rsqrt(lax.optimization_barrier(jnp.mean(reads * reads, axis=-1, keepdims=True)) + EPS)
    gate = jax.nn.silu(result_switch_preactivation.reshape(row_count, head_count, value_width).astype(jnp.float32))
    return (reads * scale * result_scaling_vector * gate).astype(jnp.bfloat16).reshape(row_count, head_count * value_width)

def slot_table(flat_route, picks, experts, capacity):
    chosen = (flat_route[:, None] == lax.broadcasted_iota(jnp.int32, (1, experts), 1)).astype(jnp.int32)
    earlier = jnp.cumsum(chosen, axis=0) - chosen
    position = lax.optimization_barrier(jnp.sum(earlier * chosen, axis=1)).astype(jnp.int32)
    source = (lax.broadcasted_iota(jnp.int32, flat_route.shape, 0) // picks).astype(jnp.int32)
    table = jnp.full((capacity * experts,), -1, jnp.int32).at[position * experts + flat_route].set(source)
    return (table.reshape(capacity, experts), position)

def fill_slots(table, normed_in):
    picked = normed_in[jnp.maximum(table, 0)]
    return jnp.where((table >= 0)[..., None], picked, jnp.zeros_like(picked))

def expert_hidden(rows_in, gate_weight, up_weight):
    gate = jnp.dot(rows_in, gate_weight, preferred_element_type=jnp.float32)
    upward = jnp.dot(rows_in, up_weight, preferred_element_type=jnp.float32)
    return (jax.nn.silu(gate) * upward).astype(jnp.bfloat16)

def expert_apply(inputs):
    rows_in, gate_weight, up_weight, down_weight = inputs
    hidden = expert_hidden(rows_in, gate_weight, up_weight)
    group = FF // N_TP
    pieces = hidden.reshape(hidden.shape[0], N_TP, group).astype(jnp.float32)
    downs = down_weight.reshape(N_TP, group, D).astype(jnp.float32)
    partial_sums = jnp.einsum('rnf,nfd->nrd', pieces, downs)
    rounded = lax.optimization_barrier(partial_sums.astype(jnp.bfloat16)).astype(jnp.float32)
    return lax.optimization_barrier(jnp.sum(rounded, axis=0)).astype(jnp.bfloat16)

def reference(initial_micro_probes, initial_micro_lookup_keys, initial_micro_payloads, result_switch_preactivation, insertion_power_preactivation, fading_preactivation, extra_fading_term, channel_fading_speed, result_scaling_vector, result_mapping_weights, latter_micro_entries, specialist_scaling_vector, selected_specialists, selected_dispatch_weights, specialist_switch_weights, specialist_expand_weights, specialist_contract_weights):
    block_count = SEQ_A // BLK
    query = to_blocks(unit_length(initial_micro_probes.reshape(SEQ_A, HEADS, DK)), block_count)
    key = to_blocks(unit_length(initial_micro_lookup_keys.reshape(SEQ_A, HEADS, DK)), block_count)
    value = to_blocks(initial_micro_payloads.reshape(SEQ_A, HEADS, DV).astype(jnp.float32), block_count)
    write = to_blocks(jax.nn.sigmoid(insertion_power_preactivation)[..., None], block_count)[..., 0]
    fading_exponent = extra_fading_term - channel_fading_speed[None, :] * jax.nn.softplus(fading_preactivation)
    fading_exponent = to_blocks(fading_exponent[..., None], block_count)[..., 0]
    terms = block_terms(query, key, value, write, fading_exponent)
    final_state, reads = lax.scan(advance, jnp.zeros((HEADS, DK, DV), jnp.float32), terms)
    reads = jnp.transpose(reads, (0, 2, 1, 3)).reshape(SEQ_A, HEADS, DV)
    normed = gated_norm(reads, result_switch_preactivation, result_scaling_vector)
    group = HEADS * DV // N_TP

    def add_group(total, index):
        columns = lax.dynamic_slice_in_dim(normed, index * group, group, 1)
        weight_rows = lax.dynamic_slice_in_dim(result_mapping_weights, index * group, group, 0)
        product = jnp.dot(columns, weight_rows, preferred_element_type=jnp.float32)
        return (total + lax.optimization_barrier(product.astype(jnp.bfloat16)).astype(jnp.float32), None)
    mixed_total, unused = lax.scan(add_group, jnp.zeros((SEQ_A, D), jnp.float32), jnp.arange(N_TP, dtype=jnp.int32))
    mixer_out = mixed_total.astype(jnp.bfloat16)
    wide_in = latter_micro_entries.astype(jnp.float32)
    normed_in = (wide_in * lax.rsqrt(lax.optimization_barrier(jnp.mean(wide_in * wide_in, axis=-1, keepdims=True)) + EPS) * specialist_scaling_vector).astype(jnp.bfloat16)
    route_blocks = selected_specialists.reshape(N_EP, TOK_MOE * TOP)
    tables, positions = jax.vmap(partial(slot_table, picks=TOP, experts=EXPERTS, capacity=CAP))(route_blocks)
    filled = jax.vmap(fill_slots)(tables, normed_in.reshape(N_EP, TOK_MOE, D))
    per_expert = jnp.transpose(filled, (2, 0, 1, 3)).reshape(EXPERTS, N_EP * CAP, D)
    results = lax.map(expert_apply, (per_expert, specialist_switch_weights, specialist_expand_weights, specialist_contract_weights))
    results = results.reshape(EXPERTS, N_EP, CAP, D)
    source_ids = lax.broadcasted_iota(jnp.int32, route_blocks.shape, 0)
    values = results[route_blocks, source_ids, positions].reshape(TOKENS_B, TOP, D)
    route_weight = selected_dispatch_weights / lax.optimization_barrier(jnp.sum(selected_dispatch_weights, axis=1, keepdims=True))
    moe_out = lax.optimization_barrier(jnp.sum(values.astype(jnp.float32) * route_weight[..., None], axis=1)).astype(jnp.bfloat16)
    return (mixer_out, moe_out)
```

```python
import functools

import jax
import jax.numpy as jnp
from jax import lax
from jax.experimental import pallas as pl
from jax.experimental.pallas import tpu as pltpu
from jax.sharding import PartitionSpec as P

BLK = 64
EPS = 1e-06
F32 = jnp.float32
BF = jnp.bfloat16
LIMIT = 60 * 1024 * 1024


def call(body, outs, flops, name, scratch=()):
    return pl.pallas_call(
        body,
        out_shape=outs,
        scratch_shapes=list(scratch),
        name=name,
        cost_estimate=pl.CostEstimate(flops=flops, bytes_accessed=1 << 21, transcendentals=0),
        compiler_params=pltpu.CompilerParams(vmem_limit_bytes=LIMIT),
    )


def mm(a, b):
    return jnp.dot(a, b, preferred_element_type=F32)


def mm_nt(a, b):
    return lax.dot_general(a, b, (((1,), (1,)), ((), ())), preferred_element_type=F32)


def mm_tn(a, b, precision=None):
    return lax.dot_general(
        a, b, (((0,), (0,)), ((), ())), preferred_element_type=F32, precision=precision
    )


def unit(x):
    return x * lax.rsqrt(jnp.sum(x * x, axis=-1, keepdims=True) + EPS)


def span_kernel(heads, q_ref, k_ref, v_ref, w_ref, f_ref, x_ref, s_ref, off_ref, map_ref, loc_ref, eff_ref):
    rows = q_ref.shape[0]
    dk = q_ref.shape[1] // heads
    dv = v_ref.shape[1] // heads
    blocks = rows // BLK
    f = f_ref[...]
    soft = jnp.maximum(f, 0.0) + jnp.log(1.0 + jnp.exp(-jnp.abs(f)))
    g = x_ref[...] - s_ref[...] * soft
    write = 1.0 / (1.0 + jnp.exp(-w_ref[...]))
    ri = lax.broadcasted_iota(jnp.int32, (BLK, BLK), 0)
    ci = lax.broadcasted_iota(jnp.int32, (BLK, BLK), 1)
    inclusive = ri >= ci
    strict = ri > ci
    tril = inclusive.astype(F32)
    triu = (ri <= ci).astype(F32)
    eye = (ri == ci).astype(F32)
    masks = []
    size = 1
    while size < BLK:
        masks.append((ri // (2 * size) == ci // (2 * size)) & (ri // size != ci // size) & strict)
        size *= 2
    hi = lax.Precision.HIGHEST
    run_c, run_r = [], []
    for b in range(blocks):
        gb = g[b * BLK : (b + 1) * BLK]
        run_c.append(jnp.dot(tril, gb, preferred_element_type=F32, precision=hi))
        run_r.append(mm_tn(gb, triu, hi))
    lows, scores, rhs, qfs, kfs, ends = [], [], [], [], [], []
    for h in range(heads):
        for b in range(blocks):
            rs = slice(b * BLK, (b + 1) * BLK)
            q = unit(q_ref[rs, h * dk : (h + 1) * dk].astype(F32))
            k = unit(k_ref[rs, h * dk : (h + 1) * dk].astype(F32))
            v = v_ref[rs, h * dv : (h + 1) * dv].astype(F32)
            kb = k.astype(BF)
            rc = run_c[b][:, h : h + 1]
            rr = run_r[b][h : h + 1, :]
            wr = write[rs, h : h + 1]
            spread = rc - rr
            fade = jnp.where(inclusive, jnp.exp(jnp.where(inclusive, spread, 0.0)), 0.0)
            lows.append(jnp.where(strict, mm_nt(kb, kb) * fade * wr, 0.0))
            scores.append((mm_nt(q.astype(BF), kb) * fade).astype(BF))
            grown = jnp.exp(rc)
            last = rc[BLK - 1 : BLK, :]
            rhs.append(jnp.concatenate([v * wr, k * (wr * grown)], axis=1).astype(BF))
            qfs.append((q * grown).astype(BF))
            kfs.append((k * jnp.exp(last - rc)).astype(BF))
            ends.append(jnp.exp(last))
    count = heads * blocks
    inv = [eye - jnp.where(masks[0], lows[i], 0.0) for i in range(count)]
    for mask in masks[1:]:
        xb = [inv[i].astype(BF) for i in range(count)]
        mid = [mm(jnp.where(mask, lows[i], 0.0).astype(BF), xb[i]).astype(BF) for i in range(count)]
        inv = [inv[i] - mm(xb[i], mid[i]) for i in range(count)]
    both = [mm(inv[i].astype(BF), rhs[i]) for i in range(count)]
    dki = lax.broadcasted_iota(jnp.int32, (dk, dk), 0)
    dkj = lax.broadcasted_iota(jnp.int32, (dk, dk), 1)
    start = jnp.concatenate([jnp.zeros((dk, dv), F32), (dki == dkj).astype(F32)], axis=1)
    state = [start for _ in range(heads)]
    zero = jnp.zeros((BLK, dk), F32)
    for b in range(blocks):
        rs = slice(b * BLK, (b + 1) * BLK)
        at = [h * blocks + b for h in range(heads)]
        sb = [state[h].astype(BF) for h in range(heads)]
        fresh = [
            (
                jnp.concatenate([both[i][:, :dv], zero], axis=1)
                - mm(both[i][:, dv:].astype(BF), sb[h])
            ).astype(BF)
            for h, i in enumerate(at)
        ]
        for h, i in enumerate(at):
            reads = mm(qfs[i], sb[h]) + mm(scores[i], fresh[h])
            loc_ref[rs, h * dv : (h + 1) * dv] = reads[:, :dv]
            eff_ref[rs, h * dk : (h + 1) * dk] = reads[:, dv:].astype(BF)
        state = [state[h] * ends[i] + mm_tn(kfs[i], fresh[h]) for h, i in enumerate(at)]
    for h in range(heads):
        off_ref[h] = state[h][:, :dv].astype(BF)
        map_ref[h] = state[h][:, dv:].astype(BF)


def fold_kernel(in_ref, out_ref):
    length, dk, width = in_ref.shape
    cols = width - dk
    state = jnp.zeros((dk, cols), F32)
    for k in range(length):
        top = state.astype(BF)
        out_ref[k] = top
        if k + 1 < length:
            rest = (state - top.astype(F32)).astype(BF)
            step = in_ref[k, :, :dk]
            state = mm(step, top) + mm(step, rest) + in_ref[k, :, dk:].astype(F32)


def project_kernel(heads, loc_ref, eff_ref, state_ref, gate_ref, gain_ref, weight_ref, out_ref, normed):
    dv = loc_ref.shape[1] // heads
    dk = eff_ref.shape[1] // heads
    for h in range(heads):
        cs = slice(h * dv, (h + 1) * dv)
        reads = loc_ref[:, cs] + mm(eff_ref[:, h * dk : (h + 1) * dk], state_ref[h])
        scale = lax.rsqrt(jnp.mean(reads * reads, axis=-1, keepdims=True) + EPS)
        gate = gate_ref[:, cs].astype(F32)
        gate = gate / (1.0 + jnp.exp(-gate))
        normed[:, cs] = (reads * scale * gain_ref[...] * gate).astype(BF)
    step = min(512, out_ref.shape[1])
    for n in range(out_ref.shape[1] // step):
        ns = slice(n * step, (n + 1) * step)
        out_ref[:, ns] = mm(normed[...], weight_ref[:, ns]).astype(BF)


def slot_places(route, experts):
    tokens, picks = route.shape
    ids = lax.broadcasted_iota(jnp.int32, (tokens, experts), 1)
    chosen = [(route[:, j : j + 1] == ids).astype(F32) for j in range(picks)]
    total = functools.reduce(jnp.add, chosen)
    ti = lax.broadcasted_iota(jnp.int32, (tokens, tokens), 0)
    tj = lax.broadcasted_iota(jnp.int32, (tokens, tokens), 1)
    before = mm((ti > tj).astype(BF), total.astype(BF))
    return [jnp.sum(before * c, axis=1, keepdims=True).astype(jnp.int32) for c in chosen]


def dispatch_kernel(experts, share, x_ref, gain_ref, route_ref, out_ref):
    x = x_ref[...].astype(F32)
    normed = (
        x * lax.rsqrt(jnp.mean(x * x, axis=-1, keepdims=True) + EPS) * gain_ref[...]
    ).astype(BF)
    route = route_ref[...]
    tokens = route.shape[0]
    first = lax.axis_index("tp") * share
    slots = lax.broadcasted_iota(jnp.int32, (tokens, experts * share), 1)
    taken = jnp.zeros((tokens, experts * share), F32)
    for j, place in enumerate(slot_places(route, experts)):
        local = place - first
        target = jnp.where((local >= 0) & (local < share), route[:, j : j + 1] * share + local, -1)
        taken = taken + (slots == target).astype(F32)
    out_ref[...] = mm_tn(taken.astype(BF), normed).astype(BF)


def combine_kernel(experts, capacity, y_ref, route_ref, score_ref, out_ref):
    route = route_ref[...]
    tokens = route.shape[0]
    score = score_ref[...]
    score = score / jnp.sum(score, axis=1, keepdims=True)
    slots = lax.broadcasted_iota(jnp.int32, (tokens, experts * capacity), 1)
    total = jnp.zeros(out_ref.shape, F32)
    for j, place in enumerate(slot_places(route, experts)):
        target = route[:, j : j + 1] * capacity + place
        total = total + score[:, j : j + 1] * mm((slots == target).astype(BF), y_ref[...])
    out_ref[...] = total.astype(BF)


def expert_kernel(x_ref, g_ref, u_ref, d_ref, out_ref, acc):
    i = pl.program_id(0)
    groups, rows, cols = out_ref.shape
    gate = mm(x_ref[...], g_ref[0])
    up = mm(x_ref[...], u_ref[0])
    hidden = (gate / (1.0 + jnp.exp(-gate)) * up).astype(BF)

    @pl.when(i == 0)
    def _():
        for n in range(groups):
            acc[n] = mm(hidden, d_ref[0, :, n * cols : (n + 1) * cols])

    @pl.when(i > 0)
    def _():
        for n in range(groups):
            acc[n] += mm(hidden, d_ref[0, :, n * cols : (n + 1) * cols])

    @pl.when(i == pl.num_programs(0) - 1)
    def _():
        for n in range(groups):
            out_ref[n] = acc[n].astype(BF)


def experts_of(x, gate, up, down, groups):
    rows, width = x.shape
    ff = gate.shape[2]
    tile = min(256, ff)
    cols = width // groups
    return pl.pallas_call(
        expert_kernel,
        grid=(ff // tile,),
        in_specs=[
            pl.BlockSpec((rows, width), lambda i: (0, 0)),
            pl.BlockSpec((1, width, tile), lambda i: (0, 0, i)),
            pl.BlockSpec((1, width, tile), lambda i: (0, 0, i)),
            pl.BlockSpec((1, tile, width), lambda i: (0, i, 0)),
        ],
        out_specs=pl.BlockSpec((groups, rows, cols), lambda i: (0, 0, 0)),
        out_shape=jax.ShapeDtypeStruct((groups, rows, cols), BF),
        scratch_shapes=[pltpu.VMEM((groups, rows, cols), F32)],
        name="experts",
        cost_estimate=pl.CostEstimate(
            flops=6 * rows * width * ff, bytes_accessed=6 * width * ff, transcendentals=rows * ff
        ),
        compiler_params=pltpu.CompilerParams(vmem_limit_bytes=LIMIT),
    )(x, gate, up, down)


def swap(value, bit, size):
    return lax.ppermute(value, "tp", [(j, j ^ bit) for j in range(size)])


def scatter_sum(parts, size):
    mine = lax.axis_index("tp")
    bit = 1
    rest = parts
    while bit < size:
        pairs = rest.reshape((rest.shape[0] // 2, 2) + rest.shape[1:])
        upper = (mine // bit) % 2
        keep = lax.dynamic_index_in_dim(pairs, upper, 1, keepdims=False)
        give = lax.dynamic_index_in_dim(pairs, 1 - upper, 1, keepdims=False)
        got = swap(give, bit, size)
        rest = (keep.astype(F32) + got.astype(F32)).astype(BF)
        bit *= 2
    return rest[0]


def gather_all(value, size):
    mine = lax.axis_index("tp")
    bit = size // 2
    rest = value[None]
    while bit >= 1:
        got = swap(rest, bit, size)
        upper = (mine // bit) % 2 == 1
        low = jnp.where(upper, got, rest)
        high = jnp.where(upper, rest, got)
        rest = jnp.stack([low, high], axis=1).reshape((2 * rest.shape[0],) + value.shape)
        bit //= 2
    return rest


def local(
    initial_micro_probes,
    initial_micro_lookup_keys,
    initial_micro_payloads,
    result_switch_preactivation,
    insertion_power_preactivation,
    fading_preactivation,
    extra_fading_term,
    channel_fading_speed,
    result_scaling_vector,
    result_mapping_weights,
    latter_micro_entries,
    specialist_scaling_vector,
    selected_specialists,
    selected_dispatch_weights,
    specialist_switch_weights,
    specialist_expand_weights,
    specialist_contract_weights,
):
    groups = lax.axis_size("tp")
    length = lax.axis_size("ep")
    rows = initial_micro_probes.shape[0]
    heads = channel_fading_speed.shape[0]
    dk = initial_micro_probes.shape[1] // heads
    dv = initial_micro_payloads.shape[1] // heads
    tokens, width = latter_micro_entries.shape
    picks = selected_specialists.shape[1]
    experts = length
    capacity = 2 * tokens * picks // experts
    share = capacity // groups
    shape = jax.ShapeDtypeStruct

    sent = call(
        functools.partial(dispatch_kernel, experts, share),
        shape((experts * share, width), BF),
        2 * tokens * experts * share * width,
        "dispatch",
    )(latter_micro_entries, specialist_scaling_vector[None], selected_specialists)
    arrived = lax.all_to_all(
        sent.reshape(experts, share, width), "ep", split_axis=0, concat_axis=0, tiled=True
    )

    offset, mapping, located, effect = call(
        functools.partial(span_kernel, heads),
        (
            shape((heads, dk, dv), BF),
            shape((heads, dk, dk), BF),
            shape((rows, heads * dv), F32),
            shape((rows, heads * dk), BF),
        ),
        12 * 10**9,
        "spans",
    )(
        initial_micro_probes,
        initial_micro_lookup_keys,
        initial_micro_payloads,
        insertion_power_preactivation,
        fading_preactivation,
        extra_fading_term,
        channel_fading_speed[None],
    )

    pieces = gather_all(arrived.reshape(experts * share, width), groups)
    partial_sums = experts_of(
        pieces.reshape(groups * experts * share, width),
        specialist_switch_weights,
        specialist_expand_weights,
        specialist_contract_weights,
        groups,
    )

    slices = length // heads
    cols = dv // slices
    cut = jnp.transpose(offset.reshape(heads, dk, slices, cols), (0, 2, 1, 3)).reshape(
        length, dk, cols
    )
    copied = jnp.broadcast_to(mapping[:, None], (heads, slices, dk, dk)).reshape(length, dk, dk)
    spans = lax.all_to_all(
        jnp.concatenate([copied, cut], axis=2), "ep", split_axis=0, concat_axis=0, tiled=True
    )
    befores = call(
        fold_kernel, shape((length, dk, cols), BF), length * 4 * dk * dk * cols, "fold"
    )(spans)
    prior = lax.all_to_all(befores, "ep", split_axis=0, concat_axis=0, tiled=True)
    prior = jnp.transpose(prior.reshape(heads, slices, dk, cols), (0, 2, 1, 3)).reshape(
        heads, dk, dv
    )
    projected = call(
        functools.partial(project_kernel, heads),
        shape((rows, result_mapping_weights.shape[1]), BF),
        2 * rows * heads * dv * result_mapping_weights.shape[1],
        "project",
        [pltpu.VMEM((rows, heads * dv), BF)],
    )(
        located,
        effect,
        prior,
        result_switch_preactivation,
        result_scaling_vector[None],
        result_mapping_weights,
    )
    mixer_out = scatter_sum(projected.reshape(groups, rows // groups, -1), groups)

    summed = scatter_sum(partial_sums, groups)
    summed = summed.reshape(groups, experts, share, width // groups)
    summed = jnp.transpose(summed, (1, 0, 2, 3)).reshape(experts, capacity, width // groups)
    returned = lax.all_to_all(summed, "ep", split_axis=0, concat_axis=0, tiled=True)
    combined = call(
        functools.partial(combine_kernel, experts, capacity),
        shape((tokens, width // groups), BF),
        4 * tokens * experts * capacity * (width // groups),
        "combine",
    )(
        returned.reshape(experts * capacity, width // groups),
        selected_specialists,
        selected_dispatch_weights,
    )
    moe_out = jnp.transpose(gather_all(combined, groups), (1, 0, 2)).reshape(tokens, width)
    return (mixer_out, moe_out)


def solution(mesh):
    return jax.shard_map(
        local,
        mesh=mesh,
        in_specs=(
            P("ep", "tp"),
            P("ep", "tp"),
            P("ep", "tp"),
            P("ep", "tp"),
            P("ep", "tp"),
            P("ep", "tp"),
            P("ep", "tp"),
            P("tp"),
            P(),
            P("tp", None),
            P("ep", None),
            P(),
            P("ep", None),
            P("ep", None),
            P("ep", None, "tp"),
            P("ep", None, "tp"),
            P("ep", "tp", None),
        ),
        out_specs=(P(("ep", "tp"), None), P("ep", None)),
        check_vma=False,
    )
```

```python
import functools

import jax
import jax.numpy as jnp
from jax import lax
from jax.experimental import pallas as pl
from jax.experimental.pallas import tpu as pltpu
from jax.sharding import PartitionSpec as P

BLK = 64
EPS = 1e-06
F32 = jnp.float32
BF = jnp.bfloat16
LIMIT = 60 * 1024 * 1024


def call(body, outs, flops, name, scratch=()):
    return pl.pallas_call(
        body,
        out_shape=outs,
        scratch_shapes=list(scratch),
        name=name,
        cost_estimate=pl.CostEstimate(flops=flops, bytes_accessed=1 << 21, transcendentals=0),
        compiler_params=pltpu.CompilerParams(vmem_limit_bytes=LIMIT),
    )


def mm(a, b):
    return jnp.dot(a, b, preferred_element_type=F32)


def mm_nt(a, b):
    return lax.dot_general(a, b, (((1,), (1,)), ((), ())), preferred_element_type=F32)


def mm_tn(a, b, precision=None):
    return lax.dot_general(
        a, b, (((0,), (0,)), ((), ())), preferred_element_type=F32, precision=precision
    )


def unit(x):
    return x * lax.rsqrt(jnp.sum(x * x, axis=-1, keepdims=True) + EPS)


def span_kernel(heads, q_ref, k_ref, v_ref, w_ref, f_ref, x_ref, s_ref, pay_ref, loc_ref, eff_ref):
    rows = q_ref.shape[0]
    dk = q_ref.shape[1] // heads
    dv = v_ref.shape[1] // heads
    blocks = rows // BLK
    f = f_ref[...]
    soft = jnp.maximum(f, 0.0) + jnp.log(1.0 + jnp.exp(-jnp.abs(f)))
    g = x_ref[...] - s_ref[...] * soft
    write = 1.0 / (1.0 + jnp.exp(-w_ref[...]))
    ri = lax.broadcasted_iota(jnp.int32, (BLK, BLK), 0)
    ci = lax.broadcasted_iota(jnp.int32, (BLK, BLK), 1)
    inclusive = ri >= ci
    strict = ri > ci
    tril = inclusive.astype(F32)
    triu = (ri <= ci).astype(F32)
    eye = (ri == ci).astype(F32)
    masks = []
    size = 1
    while size < BLK:
        masks.append((ri // (2 * size) == ci // (2 * size)) & (ri // size != ci // size) & strict)
        size *= 2
    hi = lax.Precision.HIGHEST
    run_c, run_r = [], []
    for b in range(blocks):
        gb = g[b * BLK : (b + 1) * BLK]
        run_c.append(jnp.dot(tril, gb, preferred_element_type=F32, precision=hi))
        run_r.append(mm_tn(gb, triu, hi))
    lows, scores, rhs, qfs, kfs, ends = [], [], [], [], [], []
    for h in range(heads):
        for b in range(blocks):
            rs = slice(b * BLK, (b + 1) * BLK)
            q = unit(q_ref[rs, h * dk : (h + 1) * dk].astype(F32))
            k = unit(k_ref[rs, h * dk : (h + 1) * dk].astype(F32))
            v = v_ref[rs, h * dv : (h + 1) * dv].astype(F32)
            kb = k.astype(BF)
            rc = run_c[b][:, h : h + 1]
            rr = run_r[b][h : h + 1, :]
            wr = write[rs, h : h + 1]
            spread = rc - rr
            fade = jnp.where(inclusive, jnp.exp(jnp.where(inclusive, spread, 0.0)), 0.0)
            lows.append(jnp.where(strict, mm_nt(kb, kb) * fade * wr, 0.0))
            scores.append((mm_nt(q.astype(BF), kb) * fade).astype(BF))
            grown = jnp.exp(rc)
            last = rc[BLK - 1 : BLK, :]
            rhs.append(jnp.concatenate([v * wr, k * (wr * grown)], axis=1).astype(BF))
            qfs.append((q * grown).astype(BF))
            kfs.append((k * jnp.exp(last - rc)).astype(BF))
            ends.append(jnp.exp(last))
    count = heads * blocks
    inv = [eye - jnp.where(masks[0], lows[i], 0.0) for i in range(count)]
    for mask in masks[1:]:
        xb = [inv[i].astype(BF) for i in range(count)]
        mid = [mm(jnp.where(mask, lows[i], 0.0).astype(BF), xb[i]).astype(BF) for i in range(count)]
        inv = [inv[i] - mm(xb[i], mid[i]) for i in range(count)]
    both = [mm(inv[i].astype(BF), rhs[i]) for i in range(count)]
    dki = lax.broadcasted_iota(jnp.int32, (dk, dk), 0)
    dkj = lax.broadcasted_iota(jnp.int32, (dk, dk), 1)
    start = jnp.concatenate([jnp.zeros((dk, dv), F32), (dki == dkj).astype(F32)], axis=1)
    state = [start for _ in range(heads)]
    zero = jnp.zeros((BLK, dk), F32)
    for b in range(blocks):
        rs = slice(b * BLK, (b + 1) * BLK)
        at = [h * blocks + b for h in range(heads)]
        sb = [state[h].astype(BF) for h in range(heads)]
        fresh = [
            (
                jnp.concatenate([both[i][:, :dv], zero], axis=1)
                - mm(both[i][:, dv:].astype(BF), sb[h])
            ).astype(BF)
            for h, i in enumerate(at)
        ]
        for h, i in enumerate(at):
            reads = mm(qfs[i], sb[h]) + mm(scores[i], fresh[h])
            loc_ref[rs, h * dv : (h + 1) * dv] = reads[:, :dv]
            eff_ref[rs, h * dk : (h + 1) * dk] = reads[:, dv:].astype(BF)
        state = [state[h] * ends[i] + mm_tn(kfs[i], fresh[h]) for h, i in enumerate(at)]
    for h in range(heads):
        pay_ref[h] = state[h].astype(BF)


def fold_kernel(in_ref, out_ref):
    length, dk, width = in_ref.shape
    state = jnp.zeros((dk, width - dk), F32)
    for k in range(length):
        top = state.astype(BF)
        out_ref[k] = top
        if k + 1 < length:
            rest = (state - top.astype(F32)).astype(BF)
            step = in_ref[k, :, width - dk :]
            state = mm(step, top) + mm(step, rest) + in_ref[k, :, : width - dk].astype(F32)


def flipped(index, bit):
    return index + bit - 2 * bit * ((index // bit) % 2)


def remote(src, dst, send, recv, where):
    return pltpu.make_async_remote_copy(
        src_ref=src,
        dst_ref=dst,
        send_sem=send,
        recv_sem=recv,
        device_id=where,
        device_id_type=pl.DeviceIdType.MESH,
    )


def mix_kernel(
    heads, length, groups,
    sent_ref, q_ref, k_ref, v_ref, w_ref, f_ref, x_ref, s_ref,
    out_ref, prior_ref, loc_ref, eff_ref,
    held, pay, came, states, prior,
    d_send, d_recv, g_send, g_recv, b_send, b_recv, s_send, s_recv, r_send, r_recv, done,
):
    me = lax.axis_index("ep")
    mine = lax.axis_index("tp")
    slices = length // heads
    bits = []
    bit = groups // 2
    while bit >= 1:
        bits.append(bit)
        bit //= 2
    barrier = pltpu.get_barrier_semaphore()
    for k in range(1, length):
        pl.semaphore_signal(
            barrier, inc=1, device_id={"ep": lax.rem(me + k, length)},
            device_id_type=pl.DeviceIdType.MESH,
        )
    for bit in bits:
        pl.semaphore_signal(
            barrier, inc=1, device_id={"tp": flipped(mine, bit)},
            device_id_type=pl.DeviceIdType.MESH,
        )
    pl.semaphore_wait(barrier, length - 1 + len(bits))

    pending = []
    far = {"tp": flipped(mine, bits[0])}
    own = remote(sent_ref.at[me], held.at[mine, me], g_send.at[0], g_recv.at[0], far)
    own.start()
    pending.append(own)
    for k in range(1, length):
        to = lax.rem(me + k, length)
        copy = remote(
            sent_ref.at[to], held.at[mine, me], d_send.at[k], d_recv.at[k], {"ep": to}
        )
        copy.start()
        pending.append(copy)
    held[mine, me] = sent_ref[me]

    span_kernel(heads, q_ref, k_ref, v_ref, w_ref, f_ref, x_ref, s_ref, pay, loc_ref, eff_ref)

    for k in range(1, length):
        source = lax.rem(me + length - k, length)
        block = held.at[mine, source]
        remote(block, block, d_send.at[k], d_recv.at[k], {"ep": source}).wait_recv()
        copy = remote(block, block, g_send.at[k], g_recv.at[k], far)
        copy.start()
        pending.append(copy)
    for k in range(1, length):
        to = lax.rem(me + k, length)
        copy = remote(pay.at[to // slices], came.at[me], s_send.at[k], s_recv.at[k], {"ep": to})
        copy.start()
        pending.append(copy)
    came[me] = pay[me // slices]
    spot = 0
    for bit in bits[1:]:
        block = held.at[mine]
        copy = remote(block, block, b_send.at[spot], b_recv.at[spot], {"tp": flipped(mine, bit)})
        copy.start()
        pending.append(copy)
        spot += 1
    for k in range(1, length):
        source = lax.rem(me + length - k, length)
        remote(
            pay.at[0], came.at[source], s_send.at[k], s_recv.at[k], {"ep": source}
        ).wait_recv()
    fold_kernel(came, states)
    head = me // slices
    prior[head] = states[me]
    for i in range(1, heads):
        to = lax.rem(me + i * slices, length)
        copy = remote(states.at[to], prior.at[head], r_send.at[i], r_recv.at[i], {"ep": to})
        copy.start()
        pending.append(copy)

    for k in range(length):
        source = lax.rem(me + length - k, length)
        block = held.at[flipped(mine, bits[0]), source]
        remote(block, block, g_send.at[k], g_recv.at[k], far).wait_recv()
    have = [flipped(mine, bits[0])]
    spot = 0
    later = len(bits) - 1
    for step, bit in enumerate(bits[1:]):
        side = {"tp": flipped(mine, bit)}
        for i, index in enumerate(have):
            block = held.at[index]
            at = later + (2 ** (step + 1) - 2 - step) + i
            copy = remote(block, block, b_send.at[at], b_recv.at[at], side)
            copy.start()
            pending.append(copy)
        arrived = []
        for i, index in enumerate([mine] + have):
            at = step if i == 0 else later + (2 ** (step + 1) - 2 - step) + i - 1
            there = flipped(index, bit)
            block = held.at[there]
            remote(block, block, b_send.at[at], b_recv.at[at], side).wait_recv()
            arrived.append(there)
        have = have + arrived
    whole = pltpu.make_async_copy(held, out_ref, done)
    whole.start()
    for i in range(1, heads):
        source = lax.rem(me + length - i * slices, length)
        remote(
            states.at[0], prior.at[source // slices], r_send.at[i], r_recv.at[i], {"ep": source}
        ).wait_recv()
    prior_ref[...] = prior[...]
    for copy in pending:
        copy.wait_send()
    whole.wait()


def project_kernel(heads, loc_ref, eff_ref, state_ref, gate_ref, gain_ref, weight_ref, out_ref, normed):
    dv = loc_ref.shape[1] // heads
    dk = eff_ref.shape[1] // heads
    for h in range(heads):
        cs = slice(h * dv, (h + 1) * dv)
        reads = loc_ref[:, cs] + mm(eff_ref[:, h * dk : (h + 1) * dk], state_ref[h])
        scale = lax.rsqrt(jnp.mean(reads * reads, axis=-1, keepdims=True) + EPS)
        gate = gate_ref[:, cs].astype(F32)
        gate = gate / (1.0 + jnp.exp(-gate))
        normed[:, cs] = (reads * scale * gain_ref[...] * gate).astype(BF)
    step = min(512, out_ref.shape[1])
    for n in range(out_ref.shape[1] // step):
        ns = slice(n * step, (n + 1) * step)
        out_ref[:, ns] = mm(normed[...], weight_ref[:, ns]).astype(BF)


def slot_places(route, experts):
    tokens, picks = route.shape
    ids = lax.broadcasted_iota(jnp.int32, (tokens, experts), 1)
    chosen = [(route[:, j : j + 1] == ids).astype(F32) for j in range(picks)]
    total = functools.reduce(jnp.add, chosen)
    ti = lax.broadcasted_iota(jnp.int32, (tokens, tokens), 0)
    tj = lax.broadcasted_iota(jnp.int32, (tokens, tokens), 1)
    before = mm((ti > tj).astype(BF), total.astype(BF))
    return [jnp.sum(before * c, axis=1, keepdims=True).astype(jnp.int32) for c in chosen]


def dispatch_kernel(experts, share, x_ref, gain_ref, route_ref, out_ref):
    x = x_ref[...].astype(F32)
    normed = (
        x * lax.rsqrt(jnp.mean(x * x, axis=-1, keepdims=True) + EPS) * gain_ref[...]
    ).astype(BF)
    route = route_ref[...]
    tokens = route.shape[0]
    first = lax.axis_index("tp") * share
    slots = lax.broadcasted_iota(jnp.int32, (tokens, experts * share), 1)
    taken = jnp.zeros((tokens, experts * share), F32)
    for j, place in enumerate(slot_places(route, experts)):
        local = place - first
        target = jnp.where((local >= 0) & (local < share), route[:, j : j + 1] * share + local, -1)
        taken = taken + (slots == target).astype(F32)
    out_ref[...] = mm_tn(taken.astype(BF), normed).astype(BF)


def combine_kernel(experts, capacity, y_ref, route_ref, score_ref, out_ref):
    route = route_ref[...]
    tokens = route.shape[0]
    score = score_ref[...]
    score = score / jnp.sum(score, axis=1, keepdims=True)
    slots = lax.broadcasted_iota(jnp.int32, (tokens, experts * capacity), 1)
    total = jnp.zeros(out_ref.shape, F32)
    for j, place in enumerate(slot_places(route, experts)):
        target = route[:, j : j + 1] * capacity + place
        total = total + score[:, j : j + 1] * mm((slots == target).astype(BF), y_ref[...])
    out_ref[...] = total.astype(BF)


def expert_kernel(x_ref, g_ref, u_ref, d_ref, out_ref, acc):
    i = pl.program_id(0)
    groups, rows, cols = out_ref.shape
    gate = mm(x_ref[...], g_ref[0])
    up = mm(x_ref[...], u_ref[0])
    hidden = (gate / (1.0 + jnp.exp(-gate)) * up).astype(BF)

    @pl.when(i == 0)
    def _():
        for n in range(groups):
            acc[n] = mm(hidden, d_ref[0, :, n * cols : (n + 1) * cols])

    @pl.when(i > 0)
    def _():
        for n in range(groups):
            acc[n] += mm(hidden, d_ref[0, :, n * cols : (n + 1) * cols])

    @pl.when(i == pl.num_programs(0) - 1)
    def _():
        for n in range(groups):
            out_ref[n] = acc[n].astype(BF)


def experts_of(x, gate, up, down, groups):
    rows, width = x.shape
    ff = gate.shape[2]
    tile = min(256, ff)
    cols = width // groups
    return pl.pallas_call(
        expert_kernel,
        grid=(ff // tile,),
        in_specs=[
            pl.BlockSpec((rows, width), lambda i: (0, 0)),
            pl.BlockSpec((1, width, tile), lambda i: (0, 0, i)),
            pl.BlockSpec((1, width, tile), lambda i: (0, 0, i)),
            pl.BlockSpec((1, tile, width), lambda i: (0, i, 0)),
        ],
        out_specs=pl.BlockSpec((groups, rows, cols), lambda i: (0, 0, 0)),
        out_shape=jax.ShapeDtypeStruct((groups, rows, cols), BF),
        scratch_shapes=[pltpu.VMEM((groups, rows, cols), F32)],
        name="experts",
        cost_estimate=pl.CostEstimate(
            flops=6 * rows * width * ff, bytes_accessed=6 * width * ff, transcendentals=rows * ff
        ),
        compiler_params=pltpu.CompilerParams(vmem_limit_bytes=LIMIT),
    )(x, gate, up, down)


def swap(value, bit, size):
    return lax.ppermute(value, "tp", [(j, j ^ bit) for j in range(size)])


def scatter_sum(parts, size):
    mine = lax.axis_index("tp")
    bit = 1
    rest = parts
    while bit < size:
        pairs = rest.reshape((rest.shape[0] // 2, 2) + rest.shape[1:])
        upper = (mine // bit) % 2
        keep = lax.dynamic_index_in_dim(pairs, upper, 1, keepdims=False)
        give = lax.dynamic_index_in_dim(pairs, 1 - upper, 1, keepdims=False)
        got = swap(give, bit, size)
        rest = (keep.astype(F32) + got.astype(F32)).astype(BF)
        bit *= 2
    return rest[0]


def gather_all(value, size):
    mine = lax.axis_index("tp")
    bit = size // 2
    rest = value[None]
    while bit >= 1:
        got = swap(rest, bit, size)
        upper = (mine // bit) % 2 == 1
        low = jnp.where(upper, got, rest)
        high = jnp.where(upper, rest, got)
        rest = jnp.stack([low, high], axis=1).reshape((2 * rest.shape[0],) + value.shape)
        bit //= 2
    return rest


def local(
    initial_micro_probes,
    initial_micro_lookup_keys,
    initial_micro_payloads,
    result_switch_preactivation,
    insertion_power_preactivation,
    fading_preactivation,
    extra_fading_term,
    channel_fading_speed,
    result_scaling_vector,
    result_mapping_weights,
    latter_micro_entries,
    specialist_scaling_vector,
    selected_specialists,
    selected_dispatch_weights,
    specialist_switch_weights,
    specialist_expand_weights,
    specialist_contract_weights,
):
    groups = lax.axis_size("tp")
    length = lax.axis_size("ep")
    rows = initial_micro_probes.shape[0]
    heads = channel_fading_speed.shape[0]
    dk = initial_micro_probes.shape[1] // heads
    dv = initial_micro_payloads.shape[1] // heads
    tokens, width = latter_micro_entries.shape
    picks = selected_specialists.shape[1]
    experts = length
    capacity = 2 * tokens * picks // experts
    share = capacity // groups
    shape = jax.ShapeDtypeStruct

    sent = call(
        functools.partial(dispatch_kernel, experts, share),
        shape((experts * share, width), BF),
        2 * tokens * experts * share * width,
        "dispatch",
    )(latter_micro_entries, specialist_scaling_vector[None], selected_specialists)
    vmem = pl.BlockSpec(memory_space=pltpu.VMEM)
    more = max(1, groups - 2)
    dma = pltpu.SemaphoreType.DMA
    pieces, prior, located, effect = pl.pallas_call(
        functools.partial(mix_kernel, heads, length, groups),
        out_shape=(
            shape((groups, experts, share, width), BF),
            shape((heads, dk, dv), BF),
            shape((rows, heads * dv), F32),
            shape((rows, heads * dk), BF),
        ),
        in_specs=[vmem] * 8,
        out_specs=(pl.BlockSpec(memory_space=pl.ANY), vmem, vmem, vmem),
        scratch_shapes=[
            pltpu.VMEM((groups, experts, share, width), BF),
            pltpu.VMEM((heads, dk, dv + dk), BF),
            pltpu.VMEM((length, dk, dv + dk), BF),
            pltpu.VMEM((length, dk, dv), BF),
            pltpu.VMEM((heads, dk, dv), BF),
            dma((length,)),
            dma((length,)),
            dma((length,)),
            dma((length,)),
            dma((more,)),
            dma((more,)),
            dma((length,)),
            dma((length,)),
            dma((heads,)),
            dma((heads,)),
            dma,
        ],
        name="mix",
        cost_estimate=pl.CostEstimate(
            flops=10**10, bytes_accessed=1 << 22, transcendentals=0
        ),
        compiler_params=pltpu.CompilerParams(
            vmem_limit_bytes=LIMIT, collective_id=0, has_side_effects=True
        ),
    )(
        sent.reshape(experts, share, width),
        initial_micro_probes,
        initial_micro_lookup_keys,
        initial_micro_payloads,
        insertion_power_preactivation,
        fading_preactivation,
        extra_fading_term,
        channel_fading_speed[None],
    )

    partial_sums = experts_of(
        pieces.reshape(groups * experts * share, width),
        specialist_switch_weights,
        specialist_expand_weights,
        specialist_contract_weights,
        groups,
    )

    projected = call(
        functools.partial(project_kernel, heads),
        shape((rows, result_mapping_weights.shape[1]), BF),
        2 * rows * heads * dv * result_mapping_weights.shape[1],
        "project",
        [pltpu.VMEM((rows, heads * dv), BF)],
    )(
        located,
        effect,
        prior,
        result_switch_preactivation,
        result_scaling_vector[None],
        result_mapping_weights,
    )
    mixer_out = scatter_sum(projected.reshape(groups, rows // groups, -1), groups)

    summed = scatter_sum(partial_sums, groups)
    summed = summed.reshape(groups, experts, share, width // groups)
    summed = jnp.transpose(summed, (1, 0, 2, 3)).reshape(experts, capacity, width // groups)
    returned = lax.all_to_all(summed, "ep", split_axis=0, concat_axis=0, tiled=True)
    combined = call(
        functools.partial(combine_kernel, experts, capacity),
        shape((tokens, width // groups), BF),
        4 * tokens * experts * capacity * (width // groups),
        "combine",
    )(
        returned.reshape(experts * capacity, width // groups),
        selected_specialists,
        selected_dispatch_weights,
    )
    moe_out = jnp.transpose(gather_all(combined, groups), (1, 0, 2)).reshape(tokens, width)
    return (mixer_out, moe_out)


def solution(mesh):
    return jax.shard_map(
        local,
        mesh=mesh,
        in_specs=(
            P("ep", "tp"),
            P("ep", "tp"),
            P("ep", "tp"),
            P("ep", "tp"),
            P("ep", "tp"),
            P("ep", "tp"),
            P("ep", "tp"),
            P("tp"),
            P(),
            P("tp", None),
            P("ep", None),
            P(),
            P("ep", None),
            P("ep", None),
            P("ep", None, "tp"),
            P("ep", None, "tp"),
            P("ep", "tp", None),
        ),
        out_specs=(P(("ep", "tp"), None), P("ep", None)),
        check_vma=False,
    )
```

```python
import functools

import jax
import jax.numpy as jnp
from jax import lax
from jax.experimental import pallas as pl
from jax.experimental.pallas import tpu as pltpu
from jax.sharding import PartitionSpec as P

BLK = 64
EPS = 1e-06
F32 = jnp.float32
BF = jnp.bfloat16
LIMIT = 60 * 1024 * 1024


def call(body, outs, flops, name, scratch=()):
    return pl.pallas_call(
        body,
        out_shape=outs,
        scratch_shapes=list(scratch),
        name=name,
        cost_estimate=pl.CostEstimate(flops=flops, bytes_accessed=1 << 21, transcendentals=0),
        compiler_params=pltpu.CompilerParams(vmem_limit_bytes=LIMIT),
    )


def mm(a, b):
    return jnp.dot(a, b, preferred_element_type=F32)


def mm_nt(a, b):
    return lax.dot_general(a, b, (((1,), (1,)), ((), ())), preferred_element_type=F32)


def mm_tn(a, b, precision=None):
    return lax.dot_general(
        a, b, (((0,), (0,)), ((), ())), preferred_element_type=F32, precision=precision
    )


def unit(x):
    return x * lax.rsqrt(jnp.sum(x * x, axis=-1, keepdims=True) + EPS)


def span_kernel(heads, q_ref, k_ref, v_ref, w_ref, f_ref, x_ref, s_ref, pay_ref, loc_ref, eff_ref):
    rows = q_ref.shape[0]
    dk = q_ref.shape[1] // heads
    dv = v_ref.shape[1] // heads
    blocks = rows // BLK
    f = f_ref[...]
    soft = jnp.maximum(f, 0.0) + jnp.log(1.0 + jnp.exp(-jnp.abs(f)))
    g = x_ref[...] - s_ref[...] * soft
    write = 1.0 / (1.0 + jnp.exp(-w_ref[...]))
    ri = lax.broadcasted_iota(jnp.int32, (BLK, BLK), 0)
    ci = lax.broadcasted_iota(jnp.int32, (BLK, BLK), 1)
    inclusive = ri >= ci
    strict = ri > ci
    tril = inclusive.astype(F32)
    triu = (ri <= ci).astype(F32)
    eye = (ri == ci).astype(F32)
    masks = []
    size = 1
    while size < BLK:
        masks.append((ri // (2 * size) == ci // (2 * size)) & (ri // size != ci // size) & strict)
        size *= 2
    hi = lax.Precision.HIGHEST
    run_c, run_r = [], []
    for b in range(blocks):
        gb = g[b * BLK : (b + 1) * BLK]
        run_c.append(jnp.dot(tril, gb, preferred_element_type=F32, precision=hi))
        run_r.append(mm_tn(gb, triu, hi))
    lows, scores, rhs, qfs, kfs, ends = [], [], [], [], [], []
    for h in range(heads):
        for b in range(blocks):
            rs = slice(b * BLK, (b + 1) * BLK)
            q = unit(q_ref[rs, h * dk : (h + 1) * dk].astype(F32))
            k = unit(k_ref[rs, h * dk : (h + 1) * dk].astype(F32))
            v = v_ref[rs, h * dv : (h + 1) * dv].astype(F32)
            kb = k.astype(BF)
            rc = run_c[b][:, h : h + 1]
            rr = run_r[b][h : h + 1, :]
            wr = write[rs, h : h + 1]
            spread = rc - rr
            fade = jnp.where(inclusive, jnp.exp(jnp.where(inclusive, spread, 0.0)), 0.0)
            lows.append(jnp.where(strict, mm_nt(kb, kb) * fade * wr, 0.0))
            scores.append((mm_nt(q.astype(BF), kb) * fade).astype(BF))
            grown = jnp.exp(rc)
            last = rc[BLK - 1 : BLK, :]
            rhs.append(jnp.concatenate([v * wr, k * (wr * grown)], axis=1).astype(BF))
            qfs.append((q * grown).astype(BF))
            kfs.append((k * jnp.exp(last - rc)).astype(BF))
            ends.append(jnp.exp(last))
    count = heads * blocks
    inv = [eye - jnp.where(masks[0], lows[i], 0.0) for i in range(count)]
    for mask in masks[1:]:
        xb = [inv[i].astype(BF) for i in range(count)]
        mid = [mm(jnp.where(mask, lows[i], 0.0).astype(BF), xb[i]).astype(BF) for i in range(count)]
        inv = [inv[i] - mm(xb[i], mid[i]) for i in range(count)]
    both = [mm(inv[i].astype(BF), rhs[i]) for i in range(count)]
    dki = lax.broadcasted_iota(jnp.int32, (dk, dk), 0)
    dkj = lax.broadcasted_iota(jnp.int32, (dk, dk), 1)
    start = jnp.concatenate([jnp.zeros((dk, dv), F32), (dki == dkj).astype(F32)], axis=1)
    state = [start for _ in range(heads)]
    zero = jnp.zeros((BLK, dk), F32)
    for b in range(blocks):
        rs = slice(b * BLK, (b + 1) * BLK)
        at = [h * blocks + b for h in range(heads)]
        sb = [state[h].astype(BF) for h in range(heads)]
        fresh = [
            (
                jnp.concatenate([both[i][:, :dv], zero], axis=1)
                - mm(both[i][:, dv:].astype(BF), sb[h])
            ).astype(BF)
            for h, i in enumerate(at)
        ]
        for h, i in enumerate(at):
            reads = mm(qfs[i], sb[h]) + mm(scores[i], fresh[h])
            loc_ref[rs, h * dv : (h + 1) * dv] = reads[:, :dv]
            eff_ref[rs, h * dk : (h + 1) * dk] = reads[:, dv:].astype(BF)
        state = [state[h] * ends[i] + mm_tn(kfs[i], fresh[h]) for h, i in enumerate(at)]
    for h in range(heads):
        pay_ref[h] = state[h].astype(BF)


def fold_kernel(in_ref, out_ref):
    length, dk, width = in_ref.shape
    state = jnp.zeros((dk, width - dk), F32)
    for k in range(length):
        top = state.astype(BF)
        out_ref[k] = top
        if k + 1 < length:
            rest = (state - top.astype(F32)).astype(BF)
            step = in_ref[k, :, width - dk :]
            state = mm(step, top) + mm(step, rest) + in_ref[k, :, : width - dk].astype(F32)


def flipped(index, bit):
    return index + bit - 2 * bit * ((index // bit) % 2)


def remote(src, dst, send, recv, where):
    return pltpu.make_async_remote_copy(
        src_ref=src,
        dst_ref=dst,
        send_sem=send,
        recv_sem=recv,
        device_id=where,
        device_id_type=pl.DeviceIdType.MESH,
    )


def mix_kernel(
    heads, length, groups,
    sent_ref, q_ref, k_ref, v_ref, w_ref, f_ref, x_ref, s_ref,
    out_ref, prior_ref, loc_ref, eff_ref,
    held, pay, came, states, prior,
    d_send, d_recv, g_send, g_recv, b_send, b_recv, s_send, s_recv, r_send, r_recv, done,
):
    me = lax.axis_index("ep")
    mine = lax.axis_index("tp")
    slices = length // heads
    bits = []
    bit = groups // 2
    while bit >= 1:
        bits.append(bit)
        bit //= 2
    barrier = pltpu.get_barrier_semaphore()
    for k in range(1, length):
        pl.semaphore_signal(
            barrier, inc=1, device_id={"ep": lax.rem(me + k, length)},
            device_id_type=pl.DeviceIdType.MESH,
        )
    for bit in bits:
        pl.semaphore_signal(
            barrier, inc=1, device_id={"tp": flipped(mine, bit)},
            device_id_type=pl.DeviceIdType.MESH,
        )
    pl.semaphore_wait(barrier, length - 1 + len(bits))

    pending = []
    far = {"tp": flipped(mine, bits[0])}
    own = remote(sent_ref.at[me], held.at[me, mine], g_send.at[0], g_recv.at[0], far)
    own.start()
    pending.append(own)
    for k in range(1, length):
        to = lax.rem(me + k, length)
        copy = remote(
            sent_ref.at[to], held.at[me, mine], d_send.at[k], d_recv.at[k], {"ep": to}
        )
        copy.start()
        pending.append(copy)
    held[me, mine] = sent_ref[me]

    span_kernel(heads, q_ref, k_ref, v_ref, w_ref, f_ref, x_ref, s_ref, pay, loc_ref, eff_ref)

    for k in range(1, length):
        source = lax.rem(me + length - k, length)
        block = held.at[source, mine]
        remote(block, block, d_send.at[k], d_recv.at[k], {"ep": source}).wait_recv()
        copy = remote(block, block, g_send.at[k], g_recv.at[k], far)
        copy.start()
        pending.append(copy)
    for k in range(1, length):
        to = lax.rem(me + k, length)
        copy = remote(pay.at[to // slices], came.at[me], s_send.at[k], s_recv.at[k], {"ep": to})
        copy.start()
        pending.append(copy)
    came[me] = pay[me // slices]
    spot = 0
    for bit in bits[1:]:
        block = held.at[:, mine]
        copy = remote(block, block, b_send.at[spot], b_recv.at[spot], {"tp": flipped(mine, bit)})
        copy.start()
        pending.append(copy)
        spot += 1
    for k in range(1, length):
        source = lax.rem(me + length - k, length)
        remote(
            pay.at[0], came.at[source], s_send.at[k], s_recv.at[k], {"ep": source}
        ).wait_recv()
    fold_kernel(came, states)
    head = me // slices
    prior[head] = states[me]
    for i in range(1, heads):
        to = lax.rem(me + i * slices, length)
        copy = remote(states.at[to], prior.at[head], r_send.at[i], r_recv.at[i], {"ep": to})
        copy.start()
        pending.append(copy)

    for k in range(length):
        source = lax.rem(me + length - k, length)
        block = held.at[source, flipped(mine, bits[0])]
        remote(block, block, g_send.at[k], g_recv.at[k], far).wait_recv()
    have = [flipped(mine, bits[0])]
    spot = 0
    later = len(bits) - 1
    for step, bit in enumerate(bits[1:]):
        side = {"tp": flipped(mine, bit)}
        for i, index in enumerate(have):
            block = held.at[:, index]
            at = later + (2 ** (step + 1) - 2 - step) + i
            copy = remote(block, block, b_send.at[at], b_recv.at[at], side)
            copy.start()
            pending.append(copy)
        arrived = []
        for i, index in enumerate([mine] + have):
            at = step if i == 0 else later + (2 ** (step + 1) - 2 - step) + i - 1
            there = flipped(index, bit)
            block = held.at[:, there]
            remote(block, block, b_send.at[at], b_recv.at[at], side).wait_recv()
            arrived.append(there)
        have = have + arrived
    whole = pltpu.make_async_copy(held, out_ref, done)
    whole.start()
    for i in range(1, heads):
        source = lax.rem(me + length - i * slices, length)
        remote(
            states.at[0], prior.at[source // slices], r_send.at[i], r_recv.at[i], {"ep": source}
        ).wait_recv()
    prior_ref[...] = prior[...]
    for copy in pending:
        copy.wait_send()
    whole.wait()


def project_kernel(heads, loc_ref, eff_ref, state_ref, gate_ref, gain_ref, weight_ref, out_ref, normed):
    dv = loc_ref.shape[1] // heads
    dk = eff_ref.shape[1] // heads
    for h in range(heads):
        cs = slice(h * dv, (h + 1) * dv)
        reads = loc_ref[:, cs] + mm(eff_ref[:, h * dk : (h + 1) * dk], state_ref[h])
        scale = lax.rsqrt(jnp.mean(reads * reads, axis=-1, keepdims=True) + EPS)
        gate = gate_ref[:, cs].astype(F32)
        gate = gate / (1.0 + jnp.exp(-gate))
        normed[:, cs] = (reads * scale * gain_ref[...] * gate).astype(BF)
    step = min(512, out_ref.shape[1])
    for n in range(out_ref.shape[1] // step):
        ns = slice(n * step, (n + 1) * step)
        out_ref[:, ns] = mm(normed[...], weight_ref[:, ns]).astype(BF)


def slot_places(route, experts):
    tokens, picks = route.shape
    ids = lax.broadcasted_iota(jnp.int32, (tokens, experts), 1)
    chosen = [(route[:, j : j + 1] == ids).astype(F32) for j in range(picks)]
    total = functools.reduce(jnp.add, chosen)
    ti = lax.broadcasted_iota(jnp.int32, (tokens, tokens), 0)
    tj = lax.broadcasted_iota(jnp.int32, (tokens, tokens), 1)
    before = mm((ti > tj).astype(BF), total.astype(BF))
    return [jnp.sum(before * c, axis=1, keepdims=True).astype(jnp.int32) for c in chosen]


def dispatch_kernel(experts, share, x_ref, gain_ref, route_ref, out_ref):
    x = x_ref[...].astype(F32)
    normed = (
        x * lax.rsqrt(jnp.mean(x * x, axis=-1, keepdims=True) + EPS) * gain_ref[...]
    ).astype(BF)
    route = route_ref[...]
    tokens = route.shape[0]
    first = lax.axis_index("tp") * share
    slots = lax.broadcasted_iota(jnp.int32, (tokens, experts * share), 1)
    taken = jnp.zeros((tokens, experts * share), F32)
    for j, place in enumerate(slot_places(route, experts)):
        local = place - first
        target = jnp.where((local >= 0) & (local < share), route[:, j : j + 1] * share + local, -1)
        taken = taken + (slots == target).astype(F32)
    out_ref[...] = mm_tn(taken.astype(BF), normed).astype(BF)


def return_kernel(
    length, groups, capacity,
    part_ref, route_ref, score_ref, out_ref,
    gots, sums, final, came, spread,
    l_send, l_recv, r_send, r_recv, g_send, g_recv,
):
    me = lax.axis_index("ep")
    mine = lax.axis_index("tp")
    levels = len(gots)
    bits = [1 << l for l in range(levels)]
    barrier = pltpu.get_barrier_semaphore()
    for k in range(1, length):
        pl.semaphore_signal(
            barrier, inc=1, device_id={"ep": lax.rem(me + k, length)},
            device_id_type=pl.DeviceIdType.MESH,
        )
    for bit in bits:
        pl.semaphore_signal(
            barrier, inc=1, device_id={"tp": flipped(mine, bit)},
            device_id_type=pl.DeviceIdType.MESH,
        )
    pl.semaphore_wait(barrier, length - 1 + levels)
    pending = []

    def give(level, k):
        bit = bits[level]
        other = 1 - (mine // bit) % 2
        source = part_ref if level == 0 else sums[level - 1]
        at = level * length + k
        chunk = lax.rem(me + k, length)
        return remote(
            source.at[:, other, chunk], gots[level].at[:, chunk],
            l_send.at[at], l_recv.at[at], {"tp": flipped(mine, bit)},
        )

    def back(k):
        to = lax.rem(me + k, length)
        return remote(final.at[to], came.at[me], r_send.at[k], r_recv.at[k], {"ep": to})

    def begin(copy):
        copy.start()
        pending.append(copy)

    order = list(range(1, length)) + [0]
    for k in order:
        begin(give(0, k))
    for level in range(levels):
        upper = (mine // bits[level]) % 2
        source = part_ref if level == 0 else sums[level - 1]
        before = None
        for k in order:
            chunk = lax.rem(me + k, length)
            give(level, k).wait_recv()
            total = (
                source[:, upper, chunk].astype(F32) + gots[level][:, chunk].astype(F32)
            ).astype(BF)
            if level + 1 < levels:
                width = total.shape[0] // 2
                for i in range(width):
                    for j in range(2):
                        sums[level][i, j, chunk] = total[2 * i + j]
                if before is not None:
                    begin(give(level + 1, before))
            elif k == 0:
                came[me] = total[0]
            else:
                final[chunk] = total[0]
                if before is not None:
                    begin(back(before))
            before = k
            if level + 1 == levels and k == order[-2]:
                last = k
        if level + 1 < levels:
            begin(give(level + 1, before))
        elif length > 1:
            begin(back(last))

    route = route_ref[...]
    tokens = route.shape[0]
    score = score_ref[...]
    score = score / jnp.sum(score, axis=1, keepdims=True)
    slots = lax.broadcasted_iota(jnp.int32, (tokens, length * capacity), 1)
    picks = []
    for j, place in enumerate(slot_places(route, length)):
        target = route[:, j : j + 1] * capacity + place
        picks.append((slots == target).astype(BF))
    for k in range(1, length):
        source = lax.rem(me + length - k, length)
        remote(
            final.at[source], came.at[source], r_send.at[k], r_recv.at[k], {"ep": source}
        ).wait_recv()
    values = came[...].reshape(length * capacity, came.shape[2])
    total = functools.reduce(
        jnp.add, [score[:, j : j + 1] * mm(pick, values) for j, pick in enumerate(picks)]
    )
    spread[mine] = total.astype(BF)
    out_ref[:, : spread.shape[2]] = spread[mine]
    have = [mine]
    at = 0
    for bit in reversed(bits):
        side = {"tp": flipped(mine, bit)}
        arrived = []
        for index in have:
            begin(remote(spread.at[index], spread.at[index], g_send.at[at], g_recv.at[at], side))
            at += 1
        at -= len(have)
        for index in have:
            there = flipped(index, bit)
            block = spread.at[there]
            remote(block, block, g_send.at[at], g_recv.at[at], side).wait_recv()
            arrived.append(there)
            at += 1
        have = have + arrived
    cols = spread.shape[2]
    for g in range(groups):
        out_ref[:, g * cols : (g + 1) * cols] = spread[g]
    for copy in pending:
        copy.wait_send()


def expert_kernel(x_ref, g_ref, u_ref, d_ref, out_ref, acc):
    i = pl.program_id(0)
    groups, rows, cols = out_ref.shape
    gate = mm(x_ref[...], g_ref[0])
    up = mm(x_ref[...], u_ref[0])
    hidden = (gate / (1.0 + jnp.exp(-gate)) * up).astype(BF)

    @pl.when(i == 0)
    def _():
        for n in range(groups):
            acc[n] = mm(hidden, d_ref[0, :, n * cols : (n + 1) * cols])

    @pl.when(i > 0)
    def _():
        for n in range(groups):
            acc[n] += mm(hidden, d_ref[0, :, n * cols : (n + 1) * cols])

    @pl.when(i == pl.num_programs(0) - 1)
    def _():
        for n in range(groups):
            out_ref[n] = acc[n].astype(BF)


def experts_of(x, gate, up, down, groups):
    rows, width = x.shape
    ff = gate.shape[2]
    tile = min(256, ff)
    cols = width // groups
    return pl.pallas_call(
        expert_kernel,
        grid=(ff // tile,),
        in_specs=[
            pl.BlockSpec((rows, width), lambda i: (0, 0)),
            pl.BlockSpec((1, width, tile), lambda i: (0, 0, i)),
            pl.BlockSpec((1, width, tile), lambda i: (0, 0, i)),
            pl.BlockSpec((1, tile, width), lambda i: (0, i, 0)),
        ],
        out_specs=pl.BlockSpec((groups, rows, cols), lambda i: (0, 0, 0)),
        out_shape=jax.ShapeDtypeStruct((groups, rows, cols), BF),
        scratch_shapes=[pltpu.VMEM((groups, rows, cols), F32)],
        name="experts",
        cost_estimate=pl.CostEstimate(
            flops=6 * rows * width * ff, bytes_accessed=6 * width * ff, transcendentals=rows * ff
        ),
        compiler_params=pltpu.CompilerParams(vmem_limit_bytes=LIMIT),
    )(x, gate, up, down)


def swap(value, bit, size):
    return lax.ppermute(value, "tp", [(j, j ^ bit) for j in range(size)])


def scatter_sum(parts, size):
    mine = lax.axis_index("tp")
    bit = 1
    rest = parts
    while bit < size:
        pairs = rest.reshape((rest.shape[0] // 2, 2) + rest.shape[1:])
        upper = (mine // bit) % 2
        keep = lax.dynamic_index_in_dim(pairs, upper, 1, keepdims=False)
        give = lax.dynamic_index_in_dim(pairs, 1 - upper, 1, keepdims=False)
        got = swap(give, bit, size)
        rest = (keep.astype(F32) + got.astype(F32)).astype(BF)
        bit *= 2
    return rest[0]


def local(
    initial_micro_probes,
    initial_micro_lookup_keys,
    initial_micro_payloads,
    result_switch_preactivation,
    insertion_power_preactivation,
    fading_preactivation,
    extra_fading_term,
    channel_fading_speed,
    result_scaling_vector,
    result_mapping_weights,
    latter_micro_entries,
    specialist_scaling_vector,
    selected_specialists,
    selected_dispatch_weights,
    specialist_switch_weights,
    specialist_expand_weights,
    specialist_contract_weights,
):
    groups = lax.axis_size("tp")
    length = lax.axis_size("ep")
    rows = initial_micro_probes.shape[0]
    heads = channel_fading_speed.shape[0]
    dk = initial_micro_probes.shape[1] // heads
    dv = initial_micro_payloads.shape[1] // heads
    tokens, width = latter_micro_entries.shape
    picks = selected_specialists.shape[1]
    experts = length
    capacity = 2 * tokens * picks // experts
    share = capacity // groups
    shape = jax.ShapeDtypeStruct

    sent = call(
        functools.partial(dispatch_kernel, experts, share),
        shape((experts * share, width), BF),
        2 * tokens * experts * share * width,
        "dispatch",
    )(latter_micro_entries, specialist_scaling_vector[None], selected_specialists)
    vmem = pl.BlockSpec(memory_space=pltpu.VMEM)
    more = max(1, groups - 2)
    dma = pltpu.SemaphoreType.DMA
    pieces, prior, located, effect = pl.pallas_call(
        functools.partial(mix_kernel, heads, length, groups),
        out_shape=(
            shape((experts, groups, share, width), BF),
            shape((heads, dk, dv), BF),
            shape((rows, heads * dv), F32),
            shape((rows, heads * dk), BF),
        ),
        in_specs=[vmem] * 8,
        out_specs=(pl.BlockSpec(memory_space=pl.ANY), vmem, vmem, vmem),
        scratch_shapes=[
            pltpu.VMEM((experts, groups, share, width), BF),
            pltpu.VMEM((heads, dk, dv + dk), BF),
            pltpu.VMEM((length, dk, dv + dk), BF),
            pltpu.VMEM((length, dk, dv), BF),
            pltpu.VMEM((heads, dk, dv), BF),
            dma((length,)),
            dma((length,)),
            dma((length,)),
            dma((length,)),
            dma((more,)),
            dma((more,)),
            dma((length,)),
            dma((length,)),
            dma((heads,)),
            dma((heads,)),
            dma,
        ],
        name="mix",
        cost_estimate=pl.CostEstimate(
            flops=10**10, bytes_accessed=1 << 22, transcendentals=0
        ),
        compiler_params=pltpu.CompilerParams(
            vmem_limit_bytes=LIMIT, collective_id=0, has_side_effects=True
        ),
    )(
        sent.reshape(experts, share, width),
        initial_micro_probes,
        initial_micro_lookup_keys,
        initial_micro_payloads,
        insertion_power_preactivation,
        fading_preactivation,
        extra_fading_term,
        channel_fading_speed[None],
    )

    partial_sums = experts_of(
        pieces.reshape(groups * experts * share, width),
        specialist_switch_weights,
        specialist_expand_weights,
        specialist_contract_weights,
        groups,
    )

    projected = call(
        functools.partial(project_kernel, heads),
        shape((rows, result_mapping_weights.shape[1]), BF),
        2 * rows * heads * dv * result_mapping_weights.shape[1],
        "project",
        [pltpu.VMEM((rows, heads * dv), BF)],
    )(
        located,
        effect,
        prior,
        result_switch_preactivation,
        result_scaling_vector[None],
        result_mapping_weights,
    )
    mixer_out = scatter_sum(projected.reshape(groups, rows // groups, -1), groups)

    cols = width // groups
    levels = groups.bit_length() - 1
    halves = [groups >> (l + 1) for l in range(levels)]
    moe_out = pl.pallas_call(
        functools.partial(return_kernel, length, groups, capacity),
        out_shape=shape((tokens, width), BF),
        in_specs=[vmem] * 3,
        out_specs=vmem,
        scratch_shapes=[
            [pltpu.VMEM((n, experts, capacity, cols), BF) for n in halves],
            [pltpu.VMEM((n // 2, 2, experts, capacity, cols), BF) for n in halves[:-1]],
            pltpu.VMEM((experts, capacity, cols), BF),
            pltpu.VMEM((experts, capacity, cols), BF),
            pltpu.VMEM((groups, tokens, cols), BF),
            dma((levels * length,)),
            dma((levels * length,)),
            dma((length,)),
            dma((length,)),
            dma((groups,)),
            dma((groups,)),
        ],
        name="return",
        cost_estimate=pl.CostEstimate(
            flops=10**10, bytes_accessed=1 << 22, transcendentals=0
        ),
        compiler_params=pltpu.CompilerParams(
            vmem_limit_bytes=LIMIT, collective_id=1, has_side_effects=True
        ),
    )(
        partial_sums.reshape(groups // 2, 2, experts, capacity, cols),
        selected_specialists,
        selected_dispatch_weights,
    )
    return (mixer_out, moe_out)


def solution(mesh):
    return jax.shard_map(
        local,
        mesh=mesh,
        in_specs=(
            P("ep", "tp"),
            P("ep", "tp"),
            P("ep", "tp"),
            P("ep", "tp"),
            P("ep", "tp"),
            P("ep", "tp"),
            P("ep", "tp"),
            P("tp"),
            P(),
            P("tp", None),
            P("ep", None),
            P(),
            P("ep", None),
            P("ep", None),
            P("ep", None, "tp"),
            P("ep", None, "tp"),
            P("ep", "tp", None),
        ),
        out_specs=(P(("ep", "tp"), None), P("ep", None)),
        check_vma=False,
    )
```
